256 devices in a mesh: sp: 64 (over z, x, core), tp: 4 (over y).
Axes of the slice: x: 4, y: 4, z: 8, core: 2. Of those that a mesh axis runs over, the one named last changes fastest.
Arguments:
- signal: bfloat16 [8192, 1024], P('sp', 'tp'), may hold values from -6 to 6
- step_log: float32 [8192, 64], P('sp', 'tp'), may hold values from -9 to -1.9
- forget_log: float32 [8192, 64], P('sp', 'tp'), may hold values from -1.4 to 0
- damping: float32 [64, 64], P('tp'), may hold values from 0.001 to 1.6
- freq: float32 [64, 64], P('tp'), may hold values from 0 to 50.26544
- in_re: bfloat16 [64, 64, 16], P('tp'), may hold values from -1 to 1
- in_im: bfloat16 [64, 64, 16], P('tp'), may hold values from -1 to 1
- out_re: bfloat16 [64, 16, 64], P('tp'), may hold values from -4 to 4
- out_im: bfloat16 [64, 16, 64], P('tp'), may hold values from -4 to 4
- skip: float32 [1024], P('tp'), may hold values from -4 to 4
- w_out: bfloat16 [1024, 2048], P('tp'), may hold values from -0.1875 to 0.1875
- residual: bfloat16 [8192, 2048], P('sp', 'tp'), may hold values from -60 to 60
- norm_gain: bfloat16 [2048], P('tp'), may hold values from 0.099609375 to 1.8984375
- w_gate: bfloat16 [2048, 5632], P('sp', 'tp'), may hold values from -0.125 to 0.125
- w_up: bfloat16 [2048, 5632], P('sp', 'tp'), may hold values from -0.125 to 0.125
- w_down: bfloat16 [5632, 2048], P('tp', 'sp'), may hold values from -0.078125 to 0.078125
Outputs:
- output: bfloat16 [8192, 2048], P('sp', 'tp')
The draws below stay inside these ranges and needn't reach their ends.
All inputs are finite; a program needn't handle non-finite values.
Results may differ from the reference program's by a relative error of at most 0.012.
Values may be sent and summed in bfloat16 or wider, within the bound.
No kernel may reach another device: no remote copies, remote signals or barrier semaphores. Data moves between devices by JAX's collectives and lax.ppermute only.
A program may use at most 64 MiB of HBM per device.

```python
import math
import jax
import jax.numpy as jnp
from jax import lax

D = 2048
SSM_W = 1024
FF = 5632
SSM_GROUP = 16
STATE = 64
TOK_DEV = 128
GROUPS = 64
TOKENS = 8192
N_SP = 64
N_TP = 4


def slow_groups(key):
    share = 0.5
    return jax.random.bernoulli(jax.random.fold_in(key, 101), share, (GROUPS,))


def draw_step_log(key, part):
    slow = slow_groups(key)
    base = jnp.where(slow, 0.5 * jnp.log(0.035 / TOKENS), jnp.log(0.05)).astype(jnp.float32)
    blocks = jax.random.uniform(jax.random.fold_in(key, 102), (TOKENS // TOK_DEV, GROUPS), jnp.float32, -0.7, 0.7)
    spread = jnp.repeat(blocks, TOK_DEV, axis=0)
    rough = jax.random.uniform(jax.random.fold_in(key, 103), (TOKENS, GROUPS), jnp.float32, -0.35, 0.35)
    return (base[None, :] + spread + rough).astype(jnp.float32)


def draw_damping(key, part):
    slow = slow_groups(key)
    fast_rate = jnp.exp(jax.random.uniform(jax.random.fold_in(key, 104), (GROUPS, STATE), jnp.float32, math.log(0.6), math.log(1.6)))
    slow_rate = jnp.exp(jax.random.uniform(jax.random.fold_in(key, 105), (GROUPS, STATE), jnp.float32, math.log(0.2), math.log(0.8))) / jnp.sqrt(0.035 * TOKENS)
    return jnp.where(slow[:, None], slow_rate, fast_rate).astype(jnp.float32)


def draw_forget_log(key, part):
    places = jax.random.randint(jax.random.fold_in(key, 106), (3, GROUPS), 0, TOKENS)
    depth = jax.random.uniform(jax.random.fold_in(key, 107), (3, GROUPS), jnp.float32, math.log(0.65), math.log(0.8))
    positions = jnp.arange(TOKENS)[:, None, None]
    hits = positions == places[None, :, :]
    return jnp.sum(jnp.where(hits, depth[None, :, :], 0.0), axis=1).astype(jnp.float32)


def draw_residual(key, part):
    base = jnp.clip(jax.random.normal(jax.random.fold_in(key, 108), (TOKENS, D), jnp.float32), -6.0, 6.0)
    rough = jax.random.uniform(jax.random.fold_in(key, 109), (D,), jnp.float32, -0.35, 0.35)
    columns = jnp.exp(math.log(4.0) * jnp.arange(D, dtype=jnp.float32) / D + rough)
    scales = jnp.exp(jax.random.uniform(jax.random.fold_in(key, 110), (TOKENS, 1), jnp.float32, -0.35, 0.35))
    return (0.5 * base * scales * columns[None, :]).astype(jnp.bfloat16)


def levels(key, dims, pieces, least, top_value):
    level = 1.0
    for axis_at, shards_of in pieces:
        steps = jax.random.uniform(jax.random.fold_in(jax.random.fold_in(key, 6), axis_at), (shards_of,), jnp.float32, least / len(pieces), top_value / len(pieces))
        level = level * jnp.repeat(jnp.exp(steps), dims[axis_at] // shards_of).reshape((-1,) + (1,) * (len(dims) - 1 - axis_at))
    return level


def gaussian(own_key, extent, scale, reach, split=(), held_as=jnp.bfloat16):
    entries = scale * jax.random.normal(own_key, extent, jnp.float32)
    if split:
        entries = entries * levels(own_key, extent, split, -0.22, 0.18)
    return jnp.clip(entries, -reach, reach).astype(held_as)


def setup_inputs(seed: int = 0) -> dict:
    key_list = jax.random.split(jax.random.key(seed), 17)
    signal = gaussian(key_list[0], (TOKENS, SSM_W), 1.0, 6.0, ((0, 64), (1, 4)))
    step_log = draw_step_log(jax.random.fold_in(key_list[16], 71), 0)
    forget_log = draw_forget_log(jax.random.fold_in(key_list[16], 71), 0)
    damping = draw_damping(jax.random.fold_in(key_list[16], 71), 0)
    freq = jnp.clip(50.26544 * jax.random.uniform(key_list[4], (GROUPS, STATE), jnp.float32) ** levels(key_list[4], (GROUPS, STATE), ((0, 4),), -0.2, 0.2), 0.0, 50.26544)
    in_re = gaussian(key_list[5], (GROUPS, STATE, SSM_GROUP), (2 * SSM_GROUP) ** -0.5, 1.0, ((0, 4),))
    in_im = gaussian(key_list[6], (GROUPS, STATE, SSM_GROUP), (2 * SSM_GROUP) ** -0.5, 1.0, ((0, 4),))
    out_re = gaussian(key_list[7], (GROUPS, SSM_GROUP, STATE), 1.0, 4.0, ((0, 4),))
    out_im = gaussian(key_list[8], (GROUPS, SSM_GROUP, STATE), 1.0, 4.0, ((0, 4),))
    skip = gaussian(key_list[9], (SSM_W,), 1.0, 4.0, ((0, 4),), jnp.float32)
    w_out = gaussian(key_list[10], (SSM_W, D), SSM_W ** -0.5, 0.1875, ((0, 4),))
    residual = draw_residual(jax.random.fold_in(key_list[16], 71), 0)
    norm_gain = jnp.clip(1.0 + 0.18 * jax.random.normal(key_list[12], (D,), jnp.float32), 0.099609375, 1.8984375).astype(jnp.bfloat16)
    w_gate = gaussian(key_list[13], (D, FF), D ** -0.5, 0.125, ((0, 64), (1, 4)))
    w_up = gaussian(key_list[14], (D, FF), D ** -0.5, 0.125, ((0, 64), (1, 4)))
    w_down = gaussian(key_list[15], (FF, D), FF ** -0.5, 0.078125, ((0, 4), (1, 64)))
    return dict(signal=signal, step_log=step_log, forget_log=forget_log, damping=damping, freq=freq, in_re=in_re, in_im=in_im, out_re=out_re, out_im=out_im, skip=skip, w_out=w_out, residual=residual, norm_gain=norm_gain, w_gate=w_gate, w_up=w_up, w_down=w_down)


EPS = 1e-06

def state_mixer(signal, step_log, forget_log, damping, freq, in_re, in_im, out_re, out_im, skip):
    length = signal.shape[0]
    groups, states = damping.shape
    width = in_re.shape[2]
    rows = signal.astype(jnp.float32).reshape(length, groups, width)
    weight_re = in_re.astype(jnp.float32)
    weight_im = in_im.astype(jnp.float32)
    readout_real = out_re.astype(jnp.float32)
    readout_imaginary = out_im.astype(jnp.float32)
    denom = damping * damping + freq * freq

    def advance(carry, inputs):
        state_re, state_im = carry
        row, log_step, forget = inputs
        step = jnp.exp(log_step)[:, None]
        magnitude = jnp.exp(-damping * step)
        angle = freq * step
        decay_re = magnitude * jnp.cos(angle)
        decay_im = magnitude * jnp.sin(angle)
        factor_re = (-(decay_re - 1.0) * damping + decay_im * freq) / denom
        factor_im = (-decay_im * damping - (decay_re - 1.0) * freq) / denom
        keep = jnp.exp(forget)[:, None]
        source_re = jnp.einsum('gpc,gc->gp', weight_re, row, precision=lax.Precision.HIGHEST)
        source_im = jnp.einsum('gpc,gc->gp', weight_im, row, precision=lax.Precision.HIGHEST)
        drive_re = factor_re * source_re - factor_im * source_im
        drive_im = factor_re * source_im + factor_im * source_re
        following_real = keep * (decay_re * state_re - decay_im * state_im) + drive_re
        following_imaginary = keep * (decay_re * state_im + decay_im * state_re) + drive_im
        state_readout = jnp.einsum('kuy,ky->ku', readout_real, following_real, precision=lax.Precision.HIGHEST) - jnp.einsum('kuy,ky->ku', readout_imaginary, following_imaginary, precision=lax.Precision.HIGHEST)
        return ((following_real, following_imaginary), state_readout.reshape(groups * width))
    anchor = jnp.zeros((groups, states), jnp.float32)
    _, readouts = lax.scan(advance, (anchor, anchor), (rows, step_log, forget_log))
    value = readouts + skip * signal.astype(jnp.float32)
    return jax.nn.gelu(value).astype(jnp.bfloat16)

def block_sum(left, right, parts):
    span = left.shape[1] // parts
    total = jnp.zeros((left.shape[0], right.shape[1]), jnp.float32)
    for number in range(parts):
        term = jnp.dot(left[:, number * span:(number + 1) * span], right[number * span:(number + 1) * span], preferred_element_type=jnp.float32)
        rounded = lax.optimization_barrier(term.astype(jnp.bfloat16))
        total = total + rounded.astype(jnp.float32)
    return total

def reference(signal, step_log, forget_log, damping, freq, in_re, in_im, out_re, out_im, skip, w_out, residual, norm_gain, w_gate, w_up, w_down):
    mixed = state_mixer(signal, step_log, forget_log, damping, freq, in_re, in_im, out_re, out_im, skip)

    def finish(items):
        mixed_rows, resid_rows = items
        projected = block_sum(mixed_rows, w_out, N_TP)
        middle = (resid_rows.astype(jnp.float32) + projected).astype(jnp.bfloat16)
        middle_wide = middle.astype(jnp.float32)
        mean_square = lax.optimization_barrier(jnp.mean(middle_wide * middle_wide, axis=1, keepdims=True))
        normed = (middle_wide * lax.rsqrt(mean_square + EPS) * norm_gain.astype(jnp.float32)).astype(jnp.bfloat16)
        gate = jnp.dot(normed, w_gate, preferred_element_type=jnp.float32)
        up_projected = jnp.dot(normed, w_up, preferred_element_type=jnp.float32)
        hidden = (jax.nn.silu(gate) * up_projected).astype(jnp.bfloat16)
        down = block_sum(hidden, w_down, N_TP)
        return (middle_wide + 0.5 * down).astype(jnp.bfloat16)
    outputs = lax.map(finish, (mixed.reshape(N_SP, TOK_DEV, mixed.shape[1]), residual.reshape(N_SP, TOK_DEV, residual.shape[1])))
    return outputs.reshape(residual.shape)
```

```python
import functools

import jax
import jax.numpy as jnp
from jax import lax
from jax.experimental import pallas as pl
from jax.experimental.pallas import tpu as pltpu
from jax.sharding import Mesh
from jax.sharding import PartitionSpec as P

SP = ("sp_0", "sp_1", "sp_2")
EPS = 1e-06
CHUNKS = 8
F32, BF16 = jnp.float32, jnp.bfloat16
EXACT = lax.Precision.HIGHEST
TO_LAST = (((1,), (1,)), ((), ()))


def iota(shape, dim):
    return lax.broadcasted_iota(jnp.int32, shape, dim)


def ones_where(mask, dtype):
    return jnp.where(mask, 1.0, 0.0).astype(dtype)


def exact_dot(a, b):
    return jnp.dot(a, b, precision=EXACT, preferred_element_type=F32)


def dot(a, b):
    return jnp.dot(a, b, preferred_element_type=F32)


def in_three(x):
    first = x.astype(BF16)
    rest = x - first.astype(F32)
    second = rest.astype(BF16)
    third = (rest - second.astype(F32)).astype(BF16)
    return first, second, third


def token_order(length):
    run = length // CHUNKS
    row, col = iota((length, length), 0), iota((length, length), 1)
    return (row % CHUNKS) * run + row // CHUNKS == col


def small_turn(angle):
    turns = jnp.floor(angle * 0.6366197723675814 + 0.5)
    rest = angle - turns * 1.5703125
    rest = rest - turns * 4.837512969970703e-4
    rest = rest - turns * 7.549789948768648e-8
    sq = rest * rest
    sine = rest + rest * sq * (-1.6666654611e-1 + sq * (8.3321608736e-3 - sq * 1.9515295891e-4))
    drop = sq * (-0.5 + sq * (4.166664568298827e-2 + sq * (-1.388731625493765e-3 + sq * 2.443315711809948e-5)))
    quarter = turns.astype(jnp.int32) & 3
    odd = (quarter & 1) == 1
    cosine = drop + 1.0
    sin_out = jnp.where(odd, cosine, sine)
    sin_out = jnp.where(quarter >= 2, -sin_out, sin_out)
    cos_out = jnp.where(odd, sine, cosine)
    cos_out = jnp.where((quarter == 1) | (quarter == 2), -cos_out, cos_out)
    return sin_out, jnp.where(quarter == 0, drop, cos_out - 1.0)


def shrink_minus_one(x):
    u = -x
    tail = 1 / 24 + u * (1 / 120 + u * (1 / 720 + u * (1 / 5040)))
    return u * (1.0 + u * (0.5 + u * (1 / 6 + u * tail)))


def whole_turn(angle):
    sine, cosine_minus = small_turn(angle)
    return sine, cosine_minus + 1.0


def scan_kernel(
    sig_ref, step_ref, forget_ref, damp_ref, freq_ref, inre_ref, inim_ref,
    lre_ref, lim_ref, pre_ref, pim_ref, chunk_ref, send_ref, rates_ref,
    src_ref, stp_ref, kp_ref, rows_ref, last_ref,
):
    length, groups = step_ref.shape
    states = damp_ref.shape[1]
    flat = groups * states
    width = sig_ref.shape[1] // groups
    run = length // CHUNKS
    order = token_order(length)
    sig = dot(ones_where(order, BF16), sig_ref[...]).astype(BF16)
    order32 = ones_where(order, F32)
    step_log, forget_log = step_ref[...], forget_ref[...]
    step = jnp.exp(step_log)
    spread = ones_where(iota((groups, flat), 0) == iota((groups, flat), 1) // states, F32)
    stp_ref[...] = exact_dot(exact_dot(order32, step), spread)
    kp_ref[...] = exact_dot(exact_dot(order32, jnp.exp(forget_log)), spread)
    tile = ones_where(iota((states, flat), 0) == iota((states, flat), 1) % states, F32)
    damp = jnp.sum(exact_dot(damp_ref[...], tile) * spread, axis=0, keepdims=True)
    freq = jnp.sum(exact_dot(freq_ref[...], tile) * spread, axis=0, keepdims=True)
    rates_ref[0:1, :] = damp
    rates_ref[1:2, :] = freq
    inverse = 1.0 / (damp * damp + freq * freq)
    rows_ref[0:1, :] = damp
    rows_ref[1:2, :] = freq
    rows_ref[2:3, :] = damp * inverse
    rows_ref[3:4, :] = freq * inverse
    tile_c = ones_where(iota((width, groups * width), 0) == iota((width, groups * width), 1) % width, BF16)
    own = iota((flat, groups * width), 0) // states == iota((flat, groups * width), 1) // width
    for part, ref in enumerate((inre_ref, inim_ref)):
        wide = jnp.where(own, dot(ref[...], tile_c), 0.0).astype(BF16)
        src_ref[:, part * flat : (part + 1) * flat] = lax.dot_general(sig, wide, TO_LAST, preferred_element_type=F32)

    def lanes(block, carry):
        at = pl.multiple_of(block * 128, 128)
        here = pl.ds(at, 128)
        shape = (CHUNKS, 128)
        d = jnp.broadcast_to(rows_ref[0:1, here], shape)
        w = jnp.broadcast_to(rows_ref[1:2, here], shape)
        wd = jnp.broadcast_to(rows_ref[2:3, here], shape)
        wf = jnp.broadcast_to(rows_ref[3:4, here], shape)
        p_re, p_im = jnp.ones(shape, F32), jnp.zeros(shape, F32)
        l_re, l_im = jnp.zeros(shape, F32), jnp.zeros(shape, F32)
        for i in range(run):
            rows = pl.ds(i * CHUNKS, CHUNKS)
            s = stp_ref[rows, here]
            keep = kp_ref[rows, here]
            sine, cos_less = small_turn(w * s)
            less = shrink_minus_one(d * s)
            mag = less + 1.0
            z_less = less + mag * cos_less
            z_im = mag * sine
            f_re = z_im * wf - z_less * wd
            f_im = -(z_im * wd + z_less * wf)
            s_re = src_ref[rows, here]
            s_im = src_ref[rows, pl.ds(pl.multiple_of(at + flat, 128), 128)]
            a_re = keep * (z_less + 1.0)
            a_im = keep * z_im
            l_re, l_im = (
                a_re * l_re - a_im * l_im + (f_re * s_re - f_im * s_im),
                a_re * l_im + a_im * l_re + (f_re * s_im + f_im * s_re),
            )
            p_re, p_im = a_re * p_re - a_im * p_im, a_re * p_im + a_im * p_re
            lre_ref[rows, here] = l_re
            lim_ref[rows, here] = l_im
            pre_ref[rows, here] = p_re
            pim_ref[rows, here] = p_im
        sub = iota(shape, 0)

        def earlier(value, by, fill):
            return jnp.where(sub >= by, pltpu.roll(value, by, 0), fill)

        for by in (1, 2, 4):
            q_re, q_im = earlier(p_re, by, 1.0), earlier(p_im, by, 0.0)
            m_re, m_im = earlier(l_re, by, 0.0), earlier(l_im, by, 0.0)
            l_re, l_im = p_re * m_re - p_im * m_im + l_re, p_re * m_im + p_im * m_re + l_im
            p_re, p_im = p_re * q_re - p_im * q_im, p_re * q_im + p_im * q_re
        chunk_ref[0:8, here] = earlier(p_re, 1, 1.0)
        chunk_ref[8:16, here] = earlier(p_im, 1, 0.0)
        chunk_ref[16:24, here] = earlier(l_re, 1, 0.0)
        chunk_ref[24:32, here] = earlier(l_im, 1, 0.0)
        last_ref[0:1, here] = l_re[7:8, :]
        last_ref[1:2, here] = l_im[7:8, :]
        return carry

    lax.fori_loop(0, flat // 128, lanes, 0)
    sums = in_three(jnp.sum(step, axis=0, keepdims=True)) + in_three(jnp.sum(forget_log, axis=0, keepdims=True))
    third = jnp.zeros((1, flat), F32)
    for k, piece in enumerate(sums):
        third = third + dot(piece, ones_where(iota((groups, flat), 0) == iota((groups, flat), 1) - k * groups, BF16))
    send_ref[:, 0:flat] = last_ref[0:1, :].astype(BF16)
    send_ref[:, flat : 2 * flat] = last_ref[1:2, :].astype(BF16)
    send_ref[:, 2 * flat : 3 * flat] = third.astype(BF16)


def local_scan(signal, step_log, forget_log, damping, freq, in_re, in_im):
    length, groups = step_log.shape
    states = damping.shape[1]
    flat = groups * states
    wide = jax.ShapeDtypeStruct((length, flat), F32)
    return pl.pallas_call(
        scan_kernel,
        out_shape=(
            wide, wide, wide, wide,
            jax.ShapeDtypeStruct((32, flat), F32),
            jax.ShapeDtypeStruct((1, 3 * flat), BF16),
            jax.ShapeDtypeStruct((2, flat), F32),
        ),
        scratch_shapes=[
            pltpu.VMEM((length, 2 * flat), F32),
            pltpu.VMEM((length, flat), F32),
            pltpu.VMEM((length, flat), F32),
            pltpu.VMEM((8, flat), F32),
            pltpu.VMEM((8, flat), F32),
        ],
        compiler_params=pltpu.CompilerParams(vmem_limit_bytes=24 * 2**20),
        cost_estimate=pl.CostEstimate(flops=4 * 10**9, bytes_accessed=3 * 2**20, transcendentals=0),
        name="local_scan",
    )(
        signal, step_log, forget_log, damping, freq,
        in_re.reshape(flat, -1), in_im.reshape(flat, -1),
    )


def readout_kernel(
    all_ref, lre_ref, lim_ref, pre_ref, pim_ref, chunk_ref, rates_ref, sig_ref, outre_ref, outim_ref, skip_ref, wout_ref,
    part_ref,
    are_ref, aim_ref, bre_ref, bim_ref, st_ref, wide_ref,
    *, sizes,
):
    length, flat = lre_ref.shape
    devices = all_ref.shape[0]
    outs, states = outre_ref.shape
    groups = flat // states
    width = outs // groups
    n_z = sizes[0]
    inner = devices // n_z
    row, col = iota((groups * 8, flat), 0), iota((groups * 8, flat), 1)
    own = row % groups == col // states
    sums = all_ref[:, 2 * flat : 2 * flat + 128]
    step = dot(sums, ones_where(own & (row < 3 * groups), BF16))
    forget = dot(sums, ones_where(own & (row >= 3 * groups) & (row < 6 * groups), BF16))
    sine, cosine = whole_turn(rates_ref[1:2, :] * step)
    mag = jnp.exp(forget - rates_ref[0:1, :] * step)
    me = (lax.axis_index("sp_0") * sizes[1] + lax.axis_index("sp_1")) * sizes[2] + lax.axis_index("sp_2")
    place = (iota((devices, flat), 0) % n_z) * inner + iota((devices, flat), 0) // n_z
    before = place < me
    are_ref[...] = jnp.where(before, mag * cosine, 1.0)
    aim_ref[...] = jnp.where(before, mag * sine, 0.0)
    bre_ref[...] = jnp.where(before, all_ref[:, 0:flat].astype(F32), 0.0)
    bim_ref[...] = jnp.where(before, all_ref[:, flat : 2 * flat].astype(F32), 0.0)
    p_re, p_im = jnp.ones((n_z, flat), F32), jnp.zeros((n_z, flat), F32)
    l_re, l_im = jnp.zeros((n_z, flat), F32), jnp.zeros((n_z, flat), F32)
    for i in range(inner):
        rows = pl.ds(i * n_z, n_z)
        a_re, a_im = are_ref[rows, :], aim_ref[rows, :]
        l_re, l_im = a_re * l_re - a_im * l_im + bre_ref[rows, :], a_re * l_im + a_im * l_re + bim_ref[rows, :]
        p_re, p_im = a_re * p_re - a_im * p_im, a_re * p_im + a_im * p_re
    by = 1
    while by < n_z:
        q_re, q_im = pltpu.roll(p_re, by, 0), pltpu.roll(p_im, by, 0)
        m_re, m_im = pltpu.roll(l_re, by, 0), pltpu.roll(l_im, by, 0)
        l_re, l_im = p_re * m_re - p_im * m_im + l_re, p_re * m_im + p_im * m_re + l_im
        p_re, p_im = p_re * q_re - p_im * q_im, p_re * q_im + p_im * q_re
        by *= 2
    b_re = jnp.broadcast_to(l_re[n_z - 1 : n_z, :], (8, flat))
    b_im = jnp.broadcast_to(l_im[n_z - 1 : n_z, :], (8, flat))
    c_re, c_im = chunk_ref[0:8, :], chunk_ref[8:16, :]
    first_re = c_re * b_re - c_im * b_im + chunk_ref[16:24, :]
    first_im = c_re * b_im + c_im * b_re + chunk_ref[24:32, :]
    for i in range(length // 16):
        pair_re, pair_im = [], []
        for h in range(2):
            rows = pl.ds(i * 16 + h * 8, 8)
            q_re, q_im = pre_ref[rows, :], pim_ref[rows, :]
            pair_re.append(lre_ref[rows, :] + q_re * first_re - q_im * first_im)
            pair_im.append(lim_ref[rows, :] + q_re * first_im + q_im * first_re)
        rows = pl.ds(i * 16, 16)
        st_ref[rows, 0:flat] = jnp.concatenate(pair_re, axis=0).astype(BF16)
        st_ref[rows, flat : 2 * flat] = jnp.concatenate(pair_im, axis=0).astype(BF16)
    tile = ones_where(iota((states, flat), 0) == iota((states, flat), 1) % states, BF16)
    mine = iota((outs, flat), 0) // width == iota((outs, flat), 1) // states
    wide_ref[:, 0:flat] = jnp.where(mine, dot(outre_ref[...], tile), 0.0).astype(BF16)
    wide_ref[:, flat : 2 * flat] = jnp.where(mine, -dot(outim_ref[...], tile), 0.0).astype(BF16)
    order = ones_where(token_order(length), BF16)
    sig = dot(order, sig_ref[...])
    value = lax.dot_general(st_ref[...], wide_ref[...], TO_LAST, preferred_element_type=F32) + skip_ref[...] * sig
    cube = 0.7978845608028654 * (value + 0.044715 * (value * value * value))
    mixed = (0.5 * value * (1.0 + jnp.tanh(cube))).astype(BF16)
    back = lax.dot_general(order, mixed, (((0,), (0,)), ((), ())), preferred_element_type=F32).astype(BF16)
    n_part, cols = part_ref.shape[0], part_ref.shape[2]
    for k in range(n_part):
        part_ref[k] = dot(back, wout_ref[:, k * cols : (k + 1) * cols]).astype(BF16)


def readout(gathered, scanned, signal, out_re, out_im, skip, w_out, n_tp, sizes):
    lre, lim, pre, pim, chunk, rates = scanned
    length, flat = lre.shape
    devices = gathered.shape[0]
    states = out_re.shape[2]
    outs = out_re.shape[0] * out_re.shape[1]
    model = w_out.shape[1]
    return pl.pallas_call(
        functools.partial(readout_kernel, sizes=sizes),
        out_shape=jax.ShapeDtypeStruct((n_tp, length, model // n_tp), BF16),
        scratch_shapes=[pltpu.VMEM((devices, flat), F32)] * 4
        + [pltpu.VMEM((length, 2 * flat), BF16), pltpu.VMEM((outs, 2 * flat), BF16)],
        compiler_params=pltpu.CompilerParams(vmem_limit_bytes=24 * 2**20),
        cost_estimate=pl.CostEstimate(flops=4 * 10**9, bytes_accessed=4 * 2**20, transcendentals=0),
        name="readout",
    )(
        gathered, lre, lim, pre, pim, chunk, rates, signal,
        out_re.reshape(outs, states), out_im.reshape(outs, states), skip.reshape(1, outs), w_out,
    )


def middle_kernel(part_ref, res_ref, gain_ref, mid_ref):
    length = res_ref.shape[0]
    total = res_ref[...].astype(F32)
    added = part_ref[0].astype(F32)
    for k in range(1, part_ref.shape[0]):
        added = added + part_ref[k].astype(F32)
    mid_ref[0:length, :] = (total + added).astype(BF16)
    extra = mid_ref.shape[0] - length
    mid_ref[length:, :] = jnp.broadcast_to(gain_ref[...], (extra, gain_ref.shape[1]))


def middle_of(parts, residual, gain):
    length, cols = residual.shape
    return pl.pallas_call(
        middle_kernel,
        out_shape=jax.ShapeDtypeStruct((length + 16, cols), BF16),
        cost_estimate=pl.CostEstimate(flops=10**6, bytes_accessed=2**20, transcendentals=0),
        name="middle",
    )(parts, residual, gain.reshape(1, cols))


def ffn_kernel(mid_ref, wg_ref, wu_ref, wd_ref, out_ref, norm_ref, sum_ref):
    n_tp, rows, cols = mid_ref.shape
    length = rows - 16
    at = pl.program_id(0)

    @pl.when(at == 0)
    def _():
        squares = jnp.zeros((length, 1), F32)
        for k in range(n_tp):
            m = mid_ref[k, 0:length, :].astype(F32)
            squares = squares + jnp.sum(m * m, axis=1, keepdims=True)
        scale = lax.rsqrt(squares / (n_tp * cols) + EPS)
        for k in range(n_tp):
            m = mid_ref[k, 0:length, :].astype(F32)
            gain = mid_ref[k, length : length + 1, :].astype(F32)
            norm_ref[:, k * cols : (k + 1) * cols] = (m * scale * gain).astype(BF16)
        sum_ref[...] = jnp.zeros_like(sum_ref)

    gate = dot(norm_ref[...], wg_ref[...])
    up = dot(norm_ref[...], wu_ref[...])
    hidden = (gate / (1.0 + jnp.exp(-gate)) * up).astype(BF16)
    sum_ref[...] += lax.dot_general(hidden, wd_ref[...], TO_LAST, preferred_element_type=F32)

    @pl.when(at == pl.num_programs(0) - 1)
    def _():
        for k in range(n_tp):
            out_ref[k] = sum_ref[:, k * cols : (k + 1) * cols].astype(BF16)


def ffn(mid, weights, hidden):
    n_tp, rows, cols = mid.shape
    model = n_tp * cols
    block = 128
    steps = hidden // block
    return pl.pallas_call(
        ffn_kernel,
        grid=(steps,),
        in_specs=[
            pl.BlockSpec((n_tp, rows, cols), lambda i: (0, 0, 0)),
            pl.BlockSpec((model, block), lambda i: (0, i)),
            pl.BlockSpec((model, block), lambda i: (0, i + steps)),
            pl.BlockSpec((model, block), lambda i: (0, i + 2 * steps)),
        ],
        out_specs=pl.BlockSpec((n_tp, rows - 16, cols), lambda i: (0, 0, 0)),
        out_shape=jax.ShapeDtypeStruct((n_tp, rows - 16, cols), BF16),
        scratch_shapes=[pltpu.VMEM((rows - 16, model), BF16), pltpu.VMEM((rows - 16, model), F32)],
        compiler_params=pltpu.CompilerParams(vmem_limit_bytes=32 * 2**20),
        cost_estimate=pl.CostEstimate(flops=4 * 10**9, bytes_accessed=18 * 2**20, transcendentals=0),
        name="ffn",
    )(mid, weights, weights, weights)


def copy_for_each(x, axis, count):
    return lax.all_to_all(jnp.broadcast_to(x[None], (count, *x.shape)), axis, 0, 0, tiled=True)


def local(
    signal, step_log, forget_log, damping, freq, in_re, in_im, out_re, out_im, skip,
    w_out, residual, norm_gain, w_gate, w_up, w_down,
):
    sizes = tuple(lax.axis_size(a) for a in SP)
    n_sp = sizes[0] * sizes[1] * sizes[2]
    n_tp = lax.axis_size("tp")
    hidden = w_gate.shape[1]
    together = jnp.concatenate([w_gate, w_up, w_down.T], axis=1)
    weights = lax.all_gather(together, SP, axis=0, tiled=True)
    *scanned, send, rates = local_scan(signal, step_log, forget_log, damping, freq, in_re, in_im)
    gathered = copy_for_each(send, ("sp_1", "sp_2", "sp_0"), n_sp).reshape(n_sp, -1)
    parts = readout(gathered, (*scanned, rates), signal, out_re, out_im, skip, w_out, n_tp, sizes)
    parts = lax.all_to_all(parts, "tp", 0, 0, tiled=True)
    mid = middle_of(parts, residual, norm_gain)
    everyone = lax.all_gather(mid, "tp")
    down = ffn(everyone, weights, hidden)
    down = lax.all_to_all(down, "tp", 0, 0, tiled=True)
    own = mid[: residual.shape[0]].astype(F32)
    return (own + 0.5 * jnp.sum(down.astype(F32), axis=0)).astype(BF16)


def solution(mesh):
    torus = Mesh(mesh.devices.reshape(8, 4, 2, mesh.shape["tp"]), ("sp_0", "sp_1", "sp_2", "tp"))
    return jax.shard_map(
        local,
        mesh=torus,
        in_specs=(
            P(SP, "tp"), P(SP, "tp"), P(SP, "tp"),
            P("tp", None), P("tp", None),
            P("tp", None, None), P("tp", None, None), P("tp", None, None), P("tp", None, None),
            P("tp"), P("tp", None), P(SP, "tp"), P("tp"),
            P(SP, "tp"), P(SP, "tp"), P("tp", SP),
        ),
        out_specs=P(SP, "tp"),
        check_vma=False,
    )
```

```python
import functools

import jax
import jax.numpy as jnp
from jax import lax
from jax.experimental import pallas as pl
from jax.experimental.pallas import tpu as pltpu
from jax.sharding import Mesh
from jax.sharding import PartitionSpec as P


SP = ("sp_0", "sp_1", "sp_2")
EPS = 1e-06
CHUNKS = 8
F32, BF16 = jnp.float32, jnp.bfloat16
EXACT = lax.Precision.HIGHEST
TO_LAST = (((1,), (1,)), ((), ()))


def iota(shape, dim):
    return lax.broadcasted_iota(jnp.int32, shape, dim)


def ones_where(mask, dtype):
    return jnp.where(mask, 1.0, 0.0).astype(dtype)


def exact_dot(a, b):
    return jnp.dot(a, b, precision=EXACT, preferred_element_type=F32)


def dot(a, b):
    return jnp.dot(a, b, preferred_element_type=F32)


def token_order(length):
    run = length // CHUNKS
    row, col = iota((length, length), 0), iota((length, length), 1)
    return (row % CHUNKS) * run + row // CHUNKS == col


def small_turn(angle):
    turns = jnp.floor(angle * 0.6366197723675814 + 0.5)
    rest = angle - turns * 1.5703125
    rest = rest - turns * 4.837512969970703e-4
    rest = rest - turns * 7.549789948768648e-8
    sq = rest * rest
    sine = rest + rest * sq * (-1.6666654611e-1 + sq * (8.3321608736e-3 - sq * 1.9515295891e-4))
    drop = sq * (-0.5 + sq * (4.166664568298827e-2 + sq * (-1.388731625493765e-3 + sq * 2.443315711809948e-5)))
    quarter = turns.astype(jnp.int32) & 3
    odd = (quarter & 1) == 1
    cosine = drop + 1.0
    sin_out = jnp.where(odd, cosine, sine)
    sin_out = jnp.where(quarter >= 2, -sin_out, sin_out)
    cos_out = jnp.where(odd, sine, cosine)
    cos_out = jnp.where((quarter == 1) | (quarter == 2), -cos_out, cos_out)
    return sin_out, jnp.where(quarter == 0, drop, cos_out - 1.0)


def shrink_minus_one(x):
    u = -x
    tail = 1 / 24 + u * (1 / 120 + u * (1 / 720 + u * (1 / 5040)))
    return u * (1.0 + u * (0.5 + u * (1 / 6 + u * tail)))


def scan_kernel(
    sig_ref, step_ref, forget_ref, damp_ref, freq_ref, inre_ref, inim_ref,
    all_ref, chunk_ref, send_ref,
    src_ref, stp_ref, kp_ref, rows_ref, last_ref,
):
    length, groups = step_ref.shape
    states = damp_ref.shape[1]
    flat = groups * states
    width = sig_ref.shape[1] // groups
    run = length // CHUNKS
    order = token_order(length)
    sig = dot(ones_where(order, BF16), sig_ref[...]).astype(BF16)
    order32 = ones_where(order, F32)
    step_log, forget_log = step_ref[...], forget_ref[...]
    step = jnp.exp(step_log)
    spread = ones_where(iota((groups, flat), 0) == iota((groups, flat), 1) // states, F32)
    stp_ref[...] = exact_dot(exact_dot(order32, step), spread)
    kp_ref[...] = exact_dot(exact_dot(order32, jnp.exp(forget_log)), spread)
    tile = ones_where(iota((states, flat), 0) == iota((states, flat), 1) % states, F32)
    damp = jnp.sum(exact_dot(damp_ref[...], tile) * spread, axis=0, keepdims=True)
    freq = jnp.sum(exact_dot(freq_ref[...], tile) * spread, axis=0, keepdims=True)
    inverse = 1.0 / (damp * damp + freq * freq)
    rows_ref[0:1, :] = damp
    rows_ref[1:2, :] = freq
    rows_ref[2:3, :] = damp * inverse
    rows_ref[3:4, :] = freq * inverse
    tile_c = ones_where(iota((width, groups * width), 0) == iota((width, groups * width), 1) % width, BF16)
    own = iota((flat, groups * width), 0) // states == iota((flat, groups * width), 1) // width
    for part, ref in enumerate((inre_ref, inim_ref)):
        wide = jnp.where(own, dot(ref[...], tile_c), 0.0).astype(BF16)
        src_ref[:, part * flat : (part + 1) * flat] = lax.dot_general(sig, wide, TO_LAST, preferred_element_type=F32)

    def lanes(block, carry):
        at = pl.multiple_of(block * 128, 128)
        here = pl.ds(at, 128)
        shape = (CHUNKS, 128)
        d = jnp.broadcast_to(rows_ref[0:1, here], shape)
        w = jnp.broadcast_to(rows_ref[1:2, here], shape)
        wd = jnp.broadcast_to(rows_ref[2:3, here], shape)
        wf = jnp.broadcast_to(rows_ref[3:4, here], shape)
        p_re, p_im = jnp.ones(shape, F32), jnp.zeros(shape, F32)
        l_re, l_im = jnp.zeros(shape, F32), jnp.zeros(shape, F32)
        for i in range(run):
            rows = pl.ds(i * CHUNKS, CHUNKS)
            s = stp_ref[rows, here]
            keep = kp_ref[rows, here]
            sine, cos_less = small_turn(w * s)
            less = shrink_minus_one(d * s)
            mag = less + 1.0
            z_less = less + mag * cos_less
            z_im = mag * sine
            f_re = z_im * wf - z_less * wd
            f_im = -(z_im * wd + z_less * wf)
            s_re = src_ref[rows, here]
            s_im = src_ref[rows, pl.ds(pl.multiple_of(at + flat, 128), 128)]
            a_re = keep * (z_less + 1.0)
            a_im = keep * z_im
            l_re, l_im = (
                a_re * l_re - a_im * l_im + (f_re * s_re - f_im * s_im),
                a_re * l_im + a_im * l_re + (f_re * s_im + f_im * s_re),
            )
            p_re, p_im = a_re * p_re - a_im * p_im, a_re * p_im + a_im * p_re
            for k, value in enumerate((l_re, l_im, p_re, p_im)):
                all_ref[pl.ds(k * length + i * CHUNKS, CHUNKS), here] = value
        sub = iota(shape, 0)

        def earlier(value, by, fill):
            return jnp.where(sub >= by, pltpu.roll(value, by, 0), fill)

        for by in (1, 2, 4):
            q_re, q_im = earlier(p_re, by, 1.0), earlier(p_im, by, 0.0)
            m_re, m_im = earlier(l_re, by, 0.0), earlier(l_im, by, 0.0)
            l_re, l_im = p_re * m_re - p_im * m_im + l_re, p_re * m_im + p_im * m_re + l_im
            p_re, p_im = p_re * q_re - p_im * q_im, p_re * q_im + p_im * q_re
        chunk_ref[0:8, here] = earlier(p_re, 1, 1.0)
        chunk_ref[8:16, here] = earlier(p_im, 1, 0.0)
        chunk_ref[16:24, here] = earlier(l_re, 1, 0.0)
        chunk_ref[24:32, here] = earlier(l_im, 1, 0.0)
        for k, value in enumerate((p_re, p_im, l_re, l_im)):
            last_ref[pl.ds(block + 8 * k, 1), :] = value[7:8, :]
        return carry

    lax.fori_loop(0, flat // 128, lanes, 0)
    for k in range(send_ref.shape[0]):
        send_ref[k] = last_ref[...]


def local_scan(signal, step_log, forget_log, damping, freq, in_re, in_im, n_near):
    length, groups = step_log.shape
    states = damping.shape[1]
    flat = groups * states
    return pl.pallas_call(
        scan_kernel,
        out_shape=(
            jax.ShapeDtypeStruct((4 * length, flat), F32),
            jax.ShapeDtypeStruct((32, flat), F32),
            jax.ShapeDtypeStruct((n_near, 32, 128), F32),
        ),
        scratch_shapes=[
            pltpu.VMEM((length, 2 * flat), F32),
            pltpu.VMEM((length, flat), F32),
            pltpu.VMEM((length, flat), F32),
            pltpu.VMEM((8, flat), F32),
            pltpu.VMEM((32, 128), F32),
        ],
        compiler_params=pltpu.CompilerParams(vmem_limit_bytes=24 * 2**20),
        cost_estimate=pl.CostEstimate(flops=4 * 10**9, bytes_accessed=3 * 2**20, transcendentals=0),
        name="local_scan",
    )(
        signal, step_log, forget_log, damping, freq,
        in_re.reshape(flat, -1), in_im.reshape(flat, -1),
    )


def quarters(value):
    return value[0:8, :], value[8:16, :], value[16:24, :], value[24:32, :]


def joined(first, second):
    a_re, a_im, b_re, b_im = first
    c_re, c_im, d_re, d_im = second
    return (
        c_re * a_re - c_im * a_im, c_re * a_im + c_im * a_re,
        c_re * b_re - c_im * b_im + d_re, c_re * b_im + c_im * b_re + d_im,
    )


def fold_kernel(near_ref, send_ref, inside_ref):
    me = lax.axis_index("sp_1") * lax.axis_size("sp_2") + lax.axis_index("sp_2")
    one, zero = jnp.ones((8, 128), F32), jnp.zeros((8, 128), F32)
    total = inside = (one, zero, zero, zero)
    for k in range(near_ref.shape[0]):
        total = joined(total, quarters(near_ref[k]))
        passed = jnp.broadcast_to(k < me, (8, 128))
        inside = tuple(jnp.where(passed, new, old) for new, old in zip(total, inside))
    inside_ref[...] = jnp.concatenate(inside, axis=0)
    total = jnp.concatenate(total, axis=0)
    for k in range(send_ref.shape[0]):
        send_ref[k] = total


def fold(near, n_far):
    one = near.shape[1:]
    return pl.pallas_call(
        fold_kernel,
        out_shape=(jax.ShapeDtypeStruct((n_far, *one), F32), jax.ShapeDtypeStruct(one, F32)),
        cost_estimate=pl.CostEstimate(flops=10**6, bytes_accessed=2**18, transcendentals=0),
        name="fold",
    )(near)


def readout_kernel(
    far_ref, inside_ref, all_ref, chunk_ref, sig_ref, outre_ref, outim_ref, skip_ref, wout_ref,
    part_ref,
    st_ref, wide_ref,
):
    length, flat = all_ref.shape[0] // 4, all_ref.shape[1]
    outs, states = outre_ref.shape
    groups = flat // states
    width = outs // groups
    z = lax.axis_index("sp_0")
    one, zero = jnp.ones((8, 128), F32), jnp.zeros((8, 128), F32)
    before = (one, zero, zero, zero)
    for k in range(far_ref.shape[0]):
        passed = jnp.broadcast_to(k < z, (8, 128))
        before = tuple(jnp.where(passed, new, old) for new, old in zip(joined(before, quarters(far_ref[k])), before))
    _, _, t_re, t_im = joined(before, quarters(inside_ref[...]))
    b_re = jnp.concatenate([jnp.broadcast_to(t_re[r : r + 1, :], (8, 128)) for r in range(8)], axis=1)
    b_im = jnp.concatenate([jnp.broadcast_to(t_im[r : r + 1, :], (8, 128)) for r in range(8)], axis=1)
    c_re, c_im = chunk_ref[0:8, :], chunk_ref[8:16, :]
    first_re = c_re * b_re - c_im * b_im + chunk_ref[16:24, :]
    first_im = c_re * b_im + c_im * b_re + chunk_ref[24:32, :]
    for i in range(length // 16):
        pair_re, pair_im = [], []
        for h in range(2):
            l_re, l_im, q_re, q_im = (all_ref[pl.ds(k * length + i * 16 + h * 8, 8), :] for k in range(4))
            pair_re.append(l_re + q_re * first_re - q_im * first_im)
            pair_im.append(l_im + q_re * first_im + q_im * first_re)
        rows = pl.ds(i * 16, 16)
        st_ref[rows, 0:flat] = jnp.concatenate(pair_re, axis=0).astype(BF16)
        st_ref[rows, flat : 2 * flat] = jnp.concatenate(pair_im, axis=0).astype(BF16)
    tile = ones_where(iota((states, flat), 0) == iota((states, flat), 1) % states, BF16)
    mine = iota((outs, flat), 0) // width == iota((outs, flat), 1) // states
    wide_ref[:, 0:flat] = jnp.where(mine, dot(outre_ref[...], tile), 0.0).astype(BF16)
    wide_ref[:, flat : 2 * flat] = jnp.where(mine, -dot(outim_ref[...], tile), 0.0).astype(BF16)
    order = ones_where(token_order(length), BF16)
    sig = dot(order, sig_ref[...])
    value = lax.dot_general(st_ref[...], wide_ref[...], TO_LAST, preferred_element_type=F32) + skip_ref[...] * sig
    cube = 0.7978845608028654 * (value + 0.044715 * (value * value * value))
    mixed = (0.5 * value * (1.0 + jnp.tanh(cube))).astype(BF16)
    back = lax.dot_general(order, mixed, (((0,), (0,)), ((), ())), preferred_element_type=F32).astype(BF16)
    n_part, cols = part_ref.shape[0], part_ref.shape[2]
    for k in range(n_part):
        part_ref[k] = dot(back, wout_ref[:, k * cols : (k + 1) * cols]).astype(BF16)


def readout(far, inside, scanned, chunk, signal, out_re, out_im, skip, w_out, n_tp):
    length, flat = scanned.shape[0] // 4, scanned.shape[1]
    states = out_re.shape[2]
    outs = out_re.shape[0] * out_re.shape[1]
    model = w_out.shape[1]
    return pl.pallas_call(
        readout_kernel,
        out_shape=jax.ShapeDtypeStruct((n_tp, length, model // n_tp), BF16),
        scratch_shapes=[pltpu.VMEM((length, 2 * flat), BF16), pltpu.VMEM((outs, 2 * flat), BF16)],
        compiler_params=pltpu.CompilerParams(vmem_limit_bytes=24 * 2**20),
        cost_estimate=pl.CostEstimate(flops=4 * 10**9, bytes_accessed=4 * 2**20, transcendentals=0),
        name="readout",
    )(
        far, inside, scanned, chunk, signal,
        out_re.reshape(outs, states), out_im.reshape(outs, states), skip.reshape(1, outs), w_out,
    )


def middle_kernel(part_ref, res_ref, gain_ref, mid_ref):
    length = res_ref.shape[0]
    total = res_ref[...].astype(F32)
    added = part_ref[0].astype(F32)
    for k in range(1, part_ref.shape[0]):
        added = added + part_ref[k].astype(F32)
    mid_ref[0:length, :] = (total + added).astype(BF16)
    extra = mid_ref.shape[0] - length
    mid_ref[length:, :] = jnp.broadcast_to(gain_ref[...], (extra, gain_ref.shape[1]))


def middle_of(parts, residual, gain):
    length, cols = residual.shape
    return pl.pallas_call(
        middle_kernel,
        out_shape=jax.ShapeDtypeStruct((length + 16, cols), BF16),
        cost_estimate=pl.CostEstimate(flops=10**6, bytes_accessed=2**20, transcendentals=0),
        name="middle",
    )(parts, residual, gain.reshape(1, cols))


def split_kernel(wg_ref, wu_ref, wd_ref, mine_ref, other_ref, down_ref):
    half = down_ref.shape[2]
    north = lax.axis_index("sp_2") == 1
    for ref, at in ((wg_ref, 0), (wu_ref, half)):
        low, high = ref[:, 0:half], ref[:, half:]
        mine_ref[:, at : at + half] = jnp.where(north, high, low)
        other_ref[:, at : at + half] = jnp.where(north, low, high)
    for c in range(2):
        down = wd_ref[:, c * half : (c + 1) * half]
        for k in range(down_ref.shape[0] // 2):
            down_ref[2 * k + c] = down


def split(w_gate, w_up, w_down, n_x):
    rows, hidden = w_gate.shape
    half = hidden // 2
    return pl.pallas_call(
        split_kernel,
        out_shape=(
            jax.ShapeDtypeStruct((rows, hidden), BF16),
            jax.ShapeDtypeStruct((rows, hidden), BF16),
            jax.ShapeDtypeStruct((n_x * 2, rows, half), BF16),
        ),
        cost_estimate=pl.CostEstimate(flops=10**6, bytes_accessed=2**21, transcendentals=0),
        name="split",
    )(w_gate, w_up, w_down)


def norm_kernel(mid_ref, out_ref):
    n_tp, rows, cols = mid_ref.shape
    length = rows - 16
    squares = jnp.zeros((length, 1), F32)
    for k in range(n_tp):
        m = mid_ref[k, 0:length, :].astype(F32)
        squares = squares + jnp.sum(m * m, axis=1, keepdims=True)
    scale = lax.rsqrt(squares / (n_tp * cols) + EPS)
    for k in range(n_tp):
        m = mid_ref[k, 0:length, :].astype(F32)
        gain = mid_ref[k, length : length + 1, :].astype(F32)
        out_ref[:, k * cols : (k + 1) * cols] = (m * scale * gain).astype(BF16)


def norm(mid):
    n_tp, rows, cols = mid.shape
    return pl.pallas_call(
        norm_kernel,
        out_shape=jax.ShapeDtypeStruct((rows - 16, n_tp * cols), BF16),
        cost_estimate=pl.CostEstimate(flops=10**6, bytes_accessed=2**20, transcendentals=0),
        name="norm",
    )(mid)


def ffn_kernel(own_ref, other_ref, down_hbm, *refs, n_z, n_x):
    sources = refs[: n_x + 1]
    mine_ref, theirs_ref, lhs_ref, rows_ref, down_ref, sem = refs[n_x + 1 :]
    length, model = own_ref.shape
    tall, hidden2 = rows_ref.shape[1:]
    half = hidden2 // 2
    wide = model // n_z
    cols = mine_ref.shape[2]
    part = wide // n_x
    middle = tall // 2
    targets = [
        rows_ref.at[0], rows_ref.at[1], rows_ref.at[2, 0:middle, :], rows_ref.at[2, middle:tall, :], rows_ref.at[3],
    ]
    copies = [pltpu.make_async_copy(src, dst, sem.at[k]) for k, (src, dst) in enumerate(zip(sources, targets))]
    copies.append(pltpu.make_async_copy(down_hbm, down_ref, sem.at[n_x + 1]))
    for copy in copies:
        copy.start()
    x = lax.axis_index("sp_1")
    row, col = iota((wide, wide), 0), iota((wide, wide), 1)
    turned = ones_where(row == (col // part + x) % n_x * part + col % part, BF16)
    for k in range(n_z):
        at = slice(k * wide, (k + 1) * wide)
        lhs_ref[0:length, at] = dot(own_ref[:, at], turned).astype(BF16)
        lhs_ref[length:, at] = dot(other_ref[:, at], turned).astype(BF16)
    for copy in copies[:-1]:
        copy.wait()
    both = jnp.zeros((2 * length, hidden2), F32)
    for k in range(n_z):
        right = jnp.concatenate([rows_ref[j, k * part : (k + 1) * part, :] for j in range(n_x)], axis=0)
        both = both + dot(lhs_ref[:, k * wide : (k + 1) * wide], right)
    gate, up = both[:, 0:half], both[:, half:]
    hidden = (gate / (1.0 + jnp.exp(-gate)) * up).astype(BF16)
    copies[-1].wait()
    for k in range(mine_ref.shape[0]):
        down = lax.dot_general(
            hidden, down_ref[k * cols : (k + 1) * cols, :], TO_LAST, preferred_element_type=F32
        ).astype(BF16)
        mine_ref[k] = down[0:length, :]
        theirs_ref[k] = down[length:, :]


def ffn(own, other, down, rows, n_tp, n_z, n_x):
    length, model = own.shape
    shape = jax.ShapeDtypeStruct((n_tp, length, model // n_tp), BF16)
    whole = pl.BlockSpec(memory_space=pltpu.VMEM)
    far = pl.BlockSpec(memory_space=pl.ANY)
    return pl.pallas_call(
        functools.partial(ffn_kernel, n_z=n_z, n_x=n_x),
        out_shape=(shape, shape),
        in_specs=[whole, whole, far] + [far] * len(rows),
        out_specs=(whole, whole),
        scratch_shapes=[
            pltpu.VMEM((2 * length, model), BF16),
            pltpu.VMEM((n_x, *rows[0].shape), BF16),
            pltpu.VMEM(down.shape, BF16),
            pltpu.SemaphoreType.DMA((n_x + 2,)),
        ],
        compiler_params=pltpu.CompilerParams(vmem_limit_bytes=56 * 2**20),
        cost_estimate=pl.CostEstimate(flops=4 * 10**9, bytes_accessed=9 * 2**20, transcendentals=0),
        name="ffn",
    )(own, other, down, *rows)


def shift(x, axis, by):
    count = lax.axis_size(axis)
    return lax.ppermute(x, axis, [(i, (i - by) % count) for i in range(count)])


def local(
    signal, step_log, forget_log, damping, freq, in_re, in_im, out_re, out_im, skip,
    w_out, residual, norm_gain, w_gate, w_up, w_down,
):
    sizes = tuple(lax.axis_size(a) for a in SP)
    n_tp = lax.axis_size("tp")
    tie = lax.optimization_barrier
    mine, other, spread = split(w_gate, w_up, w_down.T, sizes[1])
    other = shift(other, "sp_2", 1)
    south = lax.axis_index("sp_2") == 0
    pair = jnp.concatenate([jnp.where(south, mine, other), jnp.where(south, other, mine)], axis=0)
    second = lax.all_gather(pair, "sp_0", axis=0, tiled=True)
    spread = lax.all_to_all(spread, ("sp_1", "sp_2"), 0, 0, tiled=True)
    down = lax.all_gather(spread.reshape(-1, spread.shape[2]), "sp_0", axis=0, tiled=True)
    scanned, chunk, send = local_scan(signal, step_log, forget_log, damping, freq, in_re, in_im, sizes[1] * sizes[2])
    near = lax.all_to_all(send, ("sp_1", "sp_2"), 0, 0, tiled=True)
    send, inside = fold(near, sizes[0])
    far_states = lax.all_to_all(send, "sp_0", 0, 0, tiled=True)
    second, far_states = tie((second, far_states))
    right, left = shift(second, "sp_1", 1), shift(second, "sp_1", -1)
    parts = readout(far_states, inside, scanned, chunk, signal, out_re, out_im, skip, w_out, n_tp)
    parts = lax.all_to_all(parts, "tp", 0, 0, tiled=True)
    mid = middle_of(parts, residual, norm_gain)
    everyone = lax.all_gather(mid, "tp")
    right, left, everyone = tie((right, left, everyone))
    half = right.shape[0] // 2
    low, high = shift(right[:half], "sp_1", 1), shift(left[half:], "sp_1", -1)
    normed = norm(everyone)
    partner = shift(normed, "sp_2", 1)
    own_part, other_part = ffn(
        normed, partner, down, [second, right, low, high, left], n_tp, sizes[0], sizes[1]
    )
    other_part = shift(other_part, "sp_2", 1)
    total = (own_part.astype(F32) + other_part.astype(F32)).astype(BF16)
    total = lax.all_to_all(total, "tp", 0, 0, tiled=True)
    own = mid[: residual.shape[0]].astype(F32)
    return (own + 0.5 * jnp.sum(total.astype(F32), axis=0)).astype(BF16)


def solution(mesh):
    torus = Mesh(mesh.devices.reshape(8, 4, 2, mesh.shape["tp"]), ("sp_0", "sp_1", "sp_2", "tp"))
    return jax.shard_map(
        local,
        mesh=torus,
        in_specs=(
            P(SP, "tp"), P(SP, "tp"), P(SP, "tp"),
            P("tp", None), P("tp", None),
            P("tp", None, None), P("tp", None, None), P("tp", None, None), P("tp", None, None),
            P("tp"), P("tp", None), P(SP, "tp"), P("tp"),
            P(SP, "tp"), P(SP, "tp"), P("tp", SP),
        ),
        out_specs=P(SP, "tp"),
        check_vma=False,
    )
```

```python
import functools

import jax
import jax.numpy as jnp
from jax import lax
from jax.experimental import pallas as pl
from jax.experimental.pallas import tpu as pltpu
from jax.sharding import Mesh
from jax.sharding import PartitionSpec as P


SP = ("sp_0", "sp_1", "sp_2")
EPS = 1e-06
CHUNKS = 8
F32, BF16 = jnp.float32, jnp.bfloat16
EXACT = lax.Precision.HIGHEST
TO_LAST = (((1,), (1,)), ((), ()))


def iota(shape, dim):
    return lax.broadcasted_iota(jnp.int32, shape, dim)


def ones_where(mask, dtype):
    return jnp.where(mask, 1.0, 0.0).astype(dtype)


def exact_dot(a, b):
    return jnp.dot(a, b, precision=EXACT, preferred_element_type=F32)


def dot(a, b):
    return jnp.dot(a, b, preferred_element_type=F32)


def token_order(length):
    run = length // CHUNKS
    row, col = iota((length, length), 0), iota((length, length), 1)
    return (row % CHUNKS) * run + row // CHUNKS == col


def small_turn(angle):
    turns = jnp.floor(angle * 0.6366197723675814 + 0.5)
    rest = angle - turns * 1.5703125
    rest = rest - turns * 4.837512969970703e-4
    rest = rest - turns * 7.549789948768648e-8
    sq = rest * rest
    sine = rest + rest * sq * (-1.6666654611e-1 + sq * (8.3321608736e-3 - sq * 1.9515295891e-4))
    drop = sq * (-0.5 + sq * (4.166664568298827e-2 + sq * (-1.388731625493765e-3 + sq * 2.443315711809948e-5)))
    quarter = turns.astype(jnp.int32) & 3
    odd = (quarter & 1) == 1
    cosine = drop + 1.0
    sin_out = jnp.where(odd, cosine, sine)
    sin_out = jnp.where(quarter >= 2, -sin_out, sin_out)
    cos_out = jnp.where(odd, sine, cosine)
    cos_out = jnp.where((quarter == 1) | (quarter == 2), -cos_out, cos_out)
    return sin_out, jnp.where(quarter == 0, drop, cos_out - 1.0)


def shrink_minus_one(x):
    u = -x
    tail = 1 / 24 + u * (1 / 120 + u * (1 / 720 + u * (1 / 5040)))
    return u * (1.0 + u * (0.5 + u * (1 / 6 + u * tail)))


def scan_kernel(
    sig_ref, step_ref, forget_ref, damp_ref, freq_ref, inre_ref, inim_ref,
    all_ref, chunk_ref, send_ref,
    src_ref, stp_ref, kp_ref, rows_ref, last_ref,
):
    length, groups = step_ref.shape
    states = damp_ref.shape[1]
    flat = groups * states
    width = sig_ref.shape[1] // groups
    run = length // CHUNKS
    order = token_order(length)
    sig = dot(ones_where(order, BF16), sig_ref[...]).astype(BF16)
    order32 = ones_where(order, F32)
    step_log, forget_log = step_ref[...], forget_ref[...]
    step = jnp.exp(step_log)
    spread = ones_where(iota((groups, flat), 0) == iota((groups, flat), 1) // states, F32)
    stp_ref[...] = exact_dot(exact_dot(order32, step), spread)
    kp_ref[...] = exact_dot(exact_dot(order32, jnp.exp(forget_log)), spread)
    tile = ones_where(iota((states, flat), 0) == iota((states, flat), 1) % states, F32)
    damp = jnp.sum(exact_dot(damp_ref[...], tile) * spread, axis=0, keepdims=True)
    freq = jnp.sum(exact_dot(freq_ref[...], tile) * spread, axis=0, keepdims=True)
    inverse = 1.0 / (damp * damp + freq * freq)
    rows_ref[0:1, :] = damp
    rows_ref[1:2, :] = freq
    rows_ref[2:3, :] = damp * inverse
    rows_ref[3:4, :] = freq * inverse
    tile_c = ones_where(iota((width, groups * width), 0) == iota((width, groups * width), 1) % width, BF16)
    own = iota((flat, groups * width), 0) // states == iota((flat, groups * width), 1) // width
    for part, ref in enumerate((inre_ref, inim_ref)):
        wide = jnp.where(own, dot(ref[...], tile_c), 0.0).astype(BF16)
        src_ref[:, part * flat : (part + 1) * flat] = lax.dot_general(sig, wide, TO_LAST, preferred_element_type=F32)

    def lanes(block, carry):
        at = pl.multiple_of(block * 128, 128)
        here = pl.ds(at, 128)
        shape = (CHUNKS, 128)
        d = jnp.broadcast_to(rows_ref[0:1, here], shape)
        w = jnp.broadcast_to(rows_ref[1:2, here], shape)
        wd = jnp.broadcast_to(rows_ref[2:3, here], shape)
        wf = jnp.broadcast_to(rows_ref[3:4, here], shape)
        p_re, p_im = jnp.ones(shape, F32), jnp.zeros(shape, F32)
        l_re, l_im = jnp.zeros(shape, F32), jnp.zeros(shape, F32)
        for i in range(run):
            rows = pl.ds(i * CHUNKS, CHUNKS)
            s = stp_ref[rows, here]
            keep = kp_ref[rows, here]
            sine, cos_less = small_turn(w * s)
            less = shrink_minus_one(d * s)
            mag = less + 1.0
            z_less = less + mag * cos_less
            z_im = mag * sine
            f_re = z_im * wf - z_less * wd
            f_im = -(z_im * wd + z_less * wf)
            s_re = src_ref[rows, here]
            s_im = src_ref[rows, pl.ds(pl.multiple_of(at + flat, 128), 128)]
            a_re = keep * (z_less + 1.0)
            a_im = keep * z_im
            l_re, l_im = (
                a_re * l_re - a_im * l_im + (f_re * s_re - f_im * s_im),
                a_re * l_im + a_im * l_re + (f_re * s_im + f_im * s_re),
            )
            p_re, p_im = a_re * p_re - a_im * p_im, a_re * p_im + a_im * p_re
            for k, value in enumerate((l_re, l_im, p_re, p_im)):
                all_ref[pl.ds(k * length + i * CHUNKS, CHUNKS), here] = value
        sub = iota(shape, 0)

        def earlier(value, by, fill):
            return jnp.where(sub >= by, pltpu.roll(value, by, 0), fill)

        for by in (1, 2, 4):
            q_re, q_im = earlier(p_re, by, 1.0), earlier(p_im, by, 0.0)
            m_re, m_im = earlier(l_re, by, 0.0), earlier(l_im, by, 0.0)
            l_re, l_im = p_re * m_re - p_im * m_im + l_re, p_re * m_im + p_im * m_re + l_im
            p_re, p_im = p_re * q_re - p_im * q_im, p_re * q_im + p_im * q_re
        chunk_ref[0:8, here] = earlier(p_re, 1, 1.0)
        chunk_ref[8:16, here] = earlier(p_im, 1, 0.0)
        chunk_ref[16:24, here] = earlier(l_re, 1, 0.0)
        chunk_ref[24:32, here] = earlier(l_im, 1, 0.0)
        for k, value in enumerate((p_re, p_im, l_re, l_im)):
            last_ref[pl.ds(block + 8 * k, 1), :] = value[7:8, :]
        return carry

    lax.fori_loop(0, flat // 128, lanes, 0)
    for k in range(send_ref.shape[0]):
        send_ref[k] = last_ref[...]


def local_scan(signal, step_log, forget_log, damping, freq, in_re, in_im, n_near):
    length, groups = step_log.shape
    states = damping.shape[1]
    flat = groups * states
    return pl.pallas_call(
        scan_kernel,
        out_shape=(
            jax.ShapeDtypeStruct((4 * length, flat), F32),
            jax.ShapeDtypeStruct((32, flat), F32),
            jax.ShapeDtypeStruct((n_near, 32, 128), F32),
        ),
        scratch_shapes=[
            pltpu.VMEM((length, 2 * flat), F32),
            pltpu.VMEM((length, flat), F32),
            pltpu.VMEM((length, flat), F32),
            pltpu.VMEM((8, flat), F32),
            pltpu.VMEM((32, 128), F32),
        ],
        compiler_params=pltpu.CompilerParams(vmem_limit_bytes=24 * 2**20),
        cost_estimate=pl.CostEstimate(flops=4 * 10**9, bytes_accessed=3 * 2**20, transcendentals=0),
        name="local_scan",
    )(
        signal, step_log, forget_log, damping, freq,
        in_re.reshape(flat, -1), in_im.reshape(flat, -1),
    )


def quarters(value):
    return value[0:8, :], value[8:16, :], value[16:24, :], value[24:32, :]


def joined(first, second):
    a_re, a_im, b_re, b_im = first
    c_re, c_im, d_re, d_im = second
    return (
        c_re * a_re - c_im * a_im, c_re * a_im + c_im * a_re,
        c_re * b_re - c_im * b_im + d_re, c_re * b_im + c_im * b_re + d_im,
    )


def fold_kernel(near_ref, send_ref, inside_ref):
    me = lax.axis_index("sp_1") * lax.axis_size("sp_2") + lax.axis_index("sp_2")
    one, zero = jnp.ones((8, 128), F32), jnp.zeros((8, 128), F32)
    total = inside = (one, zero, zero, zero)
    for k in range(near_ref.shape[0]):
        total = joined(total, quarters(near_ref[k]))
        passed = jnp.broadcast_to(k < me, (8, 128))
        inside = tuple(jnp.where(passed, new, old) for new, old in zip(total, inside))
    inside_ref[...] = jnp.concatenate(inside, axis=0)
    total = jnp.concatenate(total, axis=0)
    for k in range(send_ref.shape[0]):
        send_ref[k] = total


def fold(near, n_far):
    one = near.shape[1:]
    return pl.pallas_call(
        fold_kernel,
        out_shape=(jax.ShapeDtypeStruct((n_far, *one), F32), jax.ShapeDtypeStruct(one, F32)),
        compiler_params=pltpu.CompilerParams(vmem_limit_bytes=16 * 2**20),
        cost_estimate=pl.CostEstimate(flops=10**6, bytes_accessed=2**18, transcendentals=0),
        name="fold",
    )(near)


def readout_kernel(
    far_ref, inside_ref, all_ref, chunk_ref, sig_ref, outre_ref, outim_ref, skip_ref, wout_ref,
    part_ref,
    st_ref, wide_ref,
):
    length, flat = all_ref.shape[0] // 4, all_ref.shape[1]
    outs, states = outre_ref.shape
    groups = flat // states
    width = outs // groups
    z = lax.axis_index("sp_0")
    one, zero = jnp.ones((8, 128), F32), jnp.zeros((8, 128), F32)
    before = (one, zero, zero, zero)
    for k in range(far_ref.shape[0]):
        passed = jnp.broadcast_to(k < z, (8, 128))
        before = tuple(jnp.where(passed, new, old) for new, old in zip(joined(before, quarters(far_ref[k])), before))
    _, _, t_re, t_im = joined(before, quarters(inside_ref[...]))
    b_re = jnp.concatenate([jnp.broadcast_to(t_re[r : r + 1, :], (8, 128)) for r in range(8)], axis=1)
    b_im = jnp.concatenate([jnp.broadcast_to(t_im[r : r + 1, :], (8, 128)) for r in range(8)], axis=1)
    c_re, c_im = chunk_ref[0:8, :], chunk_ref[8:16, :]
    first_re = c_re * b_re - c_im * b_im + chunk_ref[16:24, :]
    first_im = c_re * b_im + c_im * b_re + chunk_ref[24:32, :]
    for i in range(length // 16):
        pair_re, pair_im = [], []
        for h in range(2):
            l_re, l_im, q_re, q_im = (all_ref[pl.ds(k * length + i * 16 + h * 8, 8), :] for k in range(4))
            pair_re.append(l_re + q_re * first_re - q_im * first_im)
            pair_im.append(l_im + q_re * first_im + q_im * first_re)
        rows = pl.ds(i * 16, 16)
        st_ref[rows, 0:flat] = jnp.concatenate(pair_re, axis=0).astype(BF16)
        st_ref[rows, flat : 2 * flat] = jnp.concatenate(pair_im, axis=0).astype(BF16)
    tile = ones_where(iota((states, flat), 0) == iota((states, flat), 1) % states, BF16)
    mine = iota((outs, flat), 0) // width == iota((outs, flat), 1) // states
    wide_ref[:, 0:flat] = jnp.where(mine, dot(outre_ref[...], tile), 0.0).astype(BF16)
    wide_ref[:, flat : 2 * flat] = jnp.where(mine, -dot(outim_ref[...], tile), 0.0).astype(BF16)
    order = ones_where(token_order(length), BF16)
    sig = dot(order, sig_ref[...])
    value = lax.dot_general(st_ref[...], wide_ref[...], TO_LAST, preferred_element_type=F32) + skip_ref[...] * sig
    cube = 0.7978845608028654 * (value + 0.044715 * (value * value * value))
    mixed = (0.5 * value * (1.0 + jnp.tanh(cube))).astype(BF16)
    back = lax.dot_general(order, mixed, (((0,), (0,)), ((), ())), preferred_element_type=F32).astype(BF16)
    n_part, cols = part_ref.shape[0], part_ref.shape[2]
    for k in range(n_part):
        part_ref[k] = dot(back, wout_ref[:, k * cols : (k + 1) * cols]).astype(BF16)


def readout(far, inside, scanned, chunk, signal, out_re, out_im, skip, w_out, n_tp):
    length, flat = scanned.shape[0] // 4, scanned.shape[1]
    states = out_re.shape[2]
    outs = out_re.shape[0] * out_re.shape[1]
    model = w_out.shape[1]
    return pl.pallas_call(
        readout_kernel,
        out_shape=jax.ShapeDtypeStruct((n_tp, length, model // n_tp), BF16),
        scratch_shapes=[pltpu.VMEM((length, 2 * flat), BF16), pltpu.VMEM((outs, 2 * flat), BF16)],
        compiler_params=pltpu.CompilerParams(vmem_limit_bytes=24 * 2**20),
        cost_estimate=pl.CostEstimate(flops=4 * 10**9, bytes_accessed=4 * 2**20, transcendentals=0),
        name="readout",
    )(
        far, inside, scanned, chunk, signal,
        out_re.reshape(outs, states), out_im.reshape(outs, states), skip.reshape(1, outs), w_out,
    )


def middle_kernel(part_ref, res_ref, gain_ref, copies_ref, mid_ref):
    length = res_ref.shape[0]
    added = part_ref[0].astype(F32)
    for k in range(1, part_ref.shape[0]):
        added = added + part_ref[k].astype(F32)
    mid = (res_ref[...].astype(F32) + added).astype(BF16)
    mid_ref[...] = mid
    n_tp, rows, cols = copies_ref.shape
    gain = jnp.broadcast_to(gain_ref[...], (rows - length, cols))
    for k in range(n_tp):
        copies_ref[k, 0:length, :] = mid
        copies_ref[k, length:, :] = gain


def middle_of(parts, residual, gain):
    length, cols = residual.shape
    return pl.pallas_call(
        middle_kernel,
        out_shape=(
            jax.ShapeDtypeStruct((parts.shape[0], length + 16, cols), BF16),
            jax.ShapeDtypeStruct((length, cols), BF16),
        ),
        compiler_params=pltpu.CompilerParams(vmem_limit_bytes=16 * 2**20),
        cost_estimate=pl.CostEstimate(flops=10**6, bytes_accessed=2**20, transcendentals=0),
        name="middle",
    )(parts, residual, gain.reshape(1, cols))


def split_kernel(wg_ref, wu_ref, wd_ref, mine_ref, other_ref, down_ref):
    half = down_ref.shape[2]
    north = lax.axis_index("sp_2") == 1
    for ref, at in ((wg_ref, 0), (wu_ref, half)):
        low, high = ref[:, 0:half], ref[:, half:]
        mine_ref[:, at : at + half] = jnp.where(north, high, low)
        other_ref[:, at : at + half] = jnp.where(north, low, high)
    for c in range(2):
        down = wd_ref[:, c * half : (c + 1) * half]
        for k in range(down_ref.shape[0] // 2):
            down_ref[2 * k + c] = down


def split(w_gate, w_up, w_down, n_x):
    rows, hidden = w_gate.shape
    half = hidden // 2
    return pl.pallas_call(
        split_kernel,
        out_shape=(
            jax.ShapeDtypeStruct((rows, hidden), BF16),
            jax.ShapeDtypeStruct((rows, hidden), BF16),
            jax.ShapeDtypeStruct((n_x * 2, rows, half), BF16),
        ),
        cost_estimate=pl.CostEstimate(flops=10**6, bytes_accessed=2**21, transcendentals=0),
        name="split",
    )(w_gate, w_up, w_down)


def fetched(sources, targets, sem):
    copies = [pltpu.make_async_copy(src, dst, sem.at[k]) for k, (src, dst) in enumerate(zip(sources, targets))]
    for copy in copies:
        copy.start()
    return copies


def most_kernel(own_ref, other_ref, *refs, n_z, n_x):
    sources, (sum_ref, last_ref, lhs_ref, rows_ref, sem) = refs[:-5], refs[-5:]
    n_tp, rows, cols = own_ref.shape
    length, model = rows - 16, n_tp * cols
    tall = rows_ref.shape[1]
    top, low = slice(0, tall // 2), slice(tall // 2, tall)
    targets = [rows_ref.at[0]] + [rows_ref.at[k, part, :] for k in (1, 2) for part in (top, low)]
    copies = fetched(sources, targets, sem)
    x, c = lax.axis_index("sp_1"), lax.axis_index("sp_2")
    wide = cols
    part = model // n_z // n_x
    row, col = iota((wide, wide), 0), iota((wide, wide), 1)
    turn, parity, inside = col // (2 * part), col % (2 * part) // part, col % part
    source = parity * (wide // 2) + (turn + x) % n_x * part + (inside + c * (part // 2)) % part
    turned = ones_where(row == source, BF16)
    for h, ref in enumerate((own_ref, other_ref)):
        squares = jnp.zeros((length, 1), F32)
        for k in range(n_tp):
            m = ref[k, 0:length, :].astype(F32)
            squares = squares + jnp.sum(m * m, axis=1, keepdims=True)
        scale = lax.rsqrt(squares / model + EPS)
        for k in range(n_tp):
            gain = ref[k, length : length + 1, :].astype(F32)
            normed = (ref[k, 0:length, :].astype(F32) * scale * gain).astype(BF16)
            out = dot(normed, turned).astype(BF16)
            for d in range(n_x):
                at = d * tall + k * 2 * part
                lhs_ref[h * length : (h + 1) * length, at : at + 2 * part] = out[:, d * 2 * part : (d + 1) * 2 * part]
    last_ref[...] = lhs_ref[:, 2 * tall : 3 * tall]
    for copy in copies:
        copy.wait()
    total = dot(lhs_ref[:, 0:tall], rows_ref[0])
    for k, d in ((1, 1), (2, 3)):
        total = total + dot(lhs_ref[:, d * tall : (d + 1) * tall], rows_ref[k])
    sum_ref[...] = total


def most_of(own, other, rows, n_z, n_x):
    n_tp, length, cols = own.shape
    length, model = length - 16, n_tp * cols
    tall, width = rows[0].shape
    whole = pl.BlockSpec(memory_space=pltpu.VMEM)
    far = pl.BlockSpec(memory_space=pl.ANY)
    return pl.pallas_call(
        functools.partial(most_kernel, n_z=n_z, n_x=n_x),
        out_shape=(
            jax.ShapeDtypeStruct((2 * length, width), F32),
            jax.ShapeDtypeStruct((2 * length, tall), BF16),
        ),
        in_specs=[whole, whole] + [far] * len(rows),
        out_specs=(whole, whole),
        scratch_shapes=[
            pltpu.VMEM((2 * length, model), BF16),
            pltpu.VMEM((3, tall, width), BF16),
            pltpu.SemaphoreType.DMA((5,)),
        ],
        compiler_params=pltpu.CompilerParams(vmem_limit_bytes=40 * 2**20),
        cost_estimate=pl.CostEstimate(flops=2 * 10**9, bytes_accessed=6 * 2**20, transcendentals=0),
        name="most",
    )(own, other, *rows)


def rest_kernel(sum_ref, last_ref, low_hbm, high_hbm, down_hbm, mine_ref, theirs_ref, rows_ref, down_ref, sem):
    half = sum_ref.shape[1] // 2
    length, cols = mine_ref.shape[1:]
    tall = rows_ref.shape[0]
    copies = fetched(
        (low_hbm, high_hbm, down_hbm),
        (rows_ref.at[0 : tall // 2, :], rows_ref.at[tall // 2 : tall, :], down_ref),
        sem,
    )
    for copy in copies[:2]:
        copy.wait()
    both = sum_ref[...] + dot(last_ref[...], rows_ref[...])
    gate, up = both[:, 0:half], both[:, half:]
    hidden = (gate / (1.0 + jnp.exp(-gate)) * up).astype(BF16)
    copies[2].wait()
    for k in range(mine_ref.shape[0]):
        down = lax.dot_general(
            hidden, down_ref[k * cols : (k + 1) * cols, :], TO_LAST, preferred_element_type=F32
        ).astype(BF16)
        mine_ref[k] = down[0:length, :]
        theirs_ref[k] = down[length:, :]


def rest_of(total, last, low, high, down, n_tp):
    length = total.shape[0] // 2
    shape = jax.ShapeDtypeStruct((n_tp, length, down.shape[0] // n_tp), BF16)
    whole = pl.BlockSpec(memory_space=pltpu.VMEM)
    far = pl.BlockSpec(memory_space=pl.ANY)
    return pl.pallas_call(
        rest_kernel,
        out_shape=(shape, shape),
        in_specs=[whole, whole, far, far, far],
        out_specs=(whole, whole),
        scratch_shapes=[
            pltpu.VMEM((2 * low.shape[0], low.shape[1]), BF16),
            pltpu.VMEM(down.shape, BF16),
            pltpu.SemaphoreType.DMA((3,)),
        ],
        compiler_params=pltpu.CompilerParams(vmem_limit_bytes=40 * 2**20),
        cost_estimate=pl.CostEstimate(flops=2 * 10**9, bytes_accessed=5 * 2**20, transcendentals=0),
        name="rest",
    )(total, last, low, high, down)


def shift(x, axis, by):
    count = lax.axis_size(axis)
    return lax.ppermute(x, axis, [(i, (i - by) % count) for i in range(count)])


def local(
    signal, step_log, forget_log, damping, freq, in_re, in_im, out_re, out_im, skip,
    w_out, residual, norm_gain, w_gate, w_up, w_down,
):
    sizes = tuple(lax.axis_size(a) for a in SP)
    n_tp = lax.axis_size("tp")
    tie = lax.optimization_barrier
    mine, other, spread = split(w_gate, w_up, w_down.T, sizes[1])
    other = shift(other, "sp_2", 1)
    pair = jnp.concatenate([mine, other], axis=0)
    second = lax.all_gather(pair, "sp_0", axis=0, tiled=True)
    spread = lax.all_to_all(spread, ("sp_1", "sp_2"), 0, 0, tiled=True)
    down = lax.all_gather(spread.reshape(-1, spread.shape[2]), "sp_0", axis=0, tiled=True)
    scanned, chunk, send = local_scan(signal, step_log, forget_log, damping, freq, in_re, in_im, sizes[1] * sizes[2])
    near = lax.all_to_all(send, ("sp_1", "sp_2"), 0, 0, tiled=True)
    send, inside = fold(near, sizes[0])
    far_states = lax.all_to_all(send, "sp_0", 0, 0, tiled=True)
    second, far_states = tie((second, far_states))
    half = second.shape[0] // 2
    top, low = second[:half], second[half:]
    right_top, left_low = shift(top, "sp_1", 1), shift(low, "sp_1", -1)
    right_low, left_top = shift(low, "sp_1", 1), shift(top, "sp_1", -1)
    parts = readout(far_states, inside, scanned, chunk, signal, out_re, out_im, skip, w_out, n_tp)
    parts = lax.all_to_all(parts, "tp", 0, 0, tiled=True)
    copies, mid = middle_of(parts, residual, norm_gain)
    right_top, left_low, copies = tie((right_top, left_low, copies))
    far_top, far_low = shift(right_top, "sp_1", 1), shift(left_low, "sp_1", -1)
    everyone = lax.all_to_all(copies, "tp", 0, 0, tiled=True)
    partner = shift(everyone, "sp_2", 1)
    everyone, down = tie((everyone, down))
    total, last = most_of(
        everyone, partner, [second, right_top, right_low, left_top, left_low], sizes[0], sizes[1]
    )
    own_part, other_part = rest_of(total, last, far_top, far_low, down, n_tp)
    other_part = shift(other_part, "sp_2", 1)
    total = (own_part.astype(F32) + other_part.astype(F32)).astype(BF16)
    total = lax.all_to_all(total, "tp", 0, 0, tiled=True)
    own = mid.astype(F32)
    return (own + 0.5 * jnp.sum(total.astype(F32), axis=0)).astype(BF16)


def solution(mesh):
    torus = Mesh(mesh.devices.reshape(8, 4, 2, mesh.shape["tp"]), ("sp_0", "sp_1", "sp_2", "tp"))
    return jax.shard_map(
        local,
        mesh=torus,
        in_specs=(
            P(SP, "tp"), P(SP, "tp"), P(SP, "tp"),
            P("tp", None), P("tp", None),
            P("tp", None, None), P("tp", None, None), P("tp", None, None), P("tp", None, None),
            P("tp"), P("tp", None), P(SP, "tp"), P("tp"),
            P(SP, "tp"), P(SP, "tp"), P("tp", SP),
        ),
        out_specs=P(SP, "tp"),
        check_vma=False,
    )
```
